32 devices in a mesh: grp: 2 (over x), sp: 4 (over z), tp: 4 (over y, core).
Axes of the slice: x: 2, y: 2, z: 4, core: 2. Of those that a mesh axis runs over, the one named last changes fastest.
Arguments:
- stream: bfloat16 [4096, 2560], P(None, ('grp', 'sp')), parts along dimension 1, may hold values from -6 to 6
- norm_gain: float32 [2, 4096], replicated, may hold values from 0.1 to 1.9
- value_weight: bfloat16 [2, 2048, 4096], P(None, 'tp'), may hold values from -0.09375 to 0.09375
- gate_weight: bfloat16 [2, 2048, 4096], P(None, 'tp'), may hold values from -0.09375 to 0.09375
- conv_kernel: float32 [2, 2048, 31], P(None, 'tp')
- conv_bias: float32 [2, 2048], P(None, 'tp'), may hold values from -3 to 3
- channel_gain: float32 [2, 2048], P(None, 'tp'), may hold values from 0.1 to 1.9
- channel_bias: float32 [2, 2048], P(None, 'tp'), may hold values from -3 to 3
- out_weight: bfloat16 [2, 4096, 2048], P(None, 'tp'), may hold values from -0.25 to 0.25
Outputs:
- result: bfloat16 [4096, 2560], P('tp', ('grp', 'sp')), parts along dimension 1
The draws below stay inside these ranges and needn't reach their ends.
There are 2 independent parts, one for each index of `grp`. The reference program is written for one: setup_inputs(seed, part) draws one part's arguments, and reference() takes and returns one part's arrays. A program takes and returns all parts, laid end to end along the dimension named above; an argument that names none is the same for every part. Nothing has to cross between parts.
All inputs are finite; a program needn't handle non-finite values.
Results may differ from the reference program's by a relative error of at most 0.012.
Values may be sent and summed in bfloat16 or wider, within the bound.
No kernel may reach another device: no remote copies, remote signals or barrier semaphores. Data moves between devices by JAX's collectives and lax.ppermute only.
A program may use at most 128 MiB of HBM per device.

```python
import math
import jax
import jax.numpy as jnp
from jax import lax

D = 4096
C = 2048
K = 31
LAYERS = 2
TOKENS = 1280


def draw_conv_kernel(key, part):
    normal_key, factor_key = jax.random.split(key)
    samples = jax.random.truncated_normal(normal_key, -4.0, 4.0, (LAYERS, C, K), jnp.float32)
    rising = 10.0 ** (jnp.arange(C, dtype=jnp.float32) / (C - 1))
    jitter = jnp.exp(jax.random.uniform(factor_key, (LAYERS, C, 1), jnp.float32, -0.35, 0.35))
    return samples * rising[None, :, None] * jitter * (0.5 / math.sqrt(K))


def steps_of(stream_key, shape, cuts, smallest, top_value):
    factor_of = 1.0
    for position, blocks in cuts:
        heights = jax.random.uniform(jax.random.fold_in(jax.random.fold_in(stream_key, 6), position), (blocks,), jnp.float32, smallest / len(cuts), top_value / len(cuts))
        factor_of = factor_of * jnp.repeat(jnp.exp(heights), shape[position] // blocks).reshape((-1,) + (1,) * (len(shape) - 1 - position))
    return factor_of


def gaussian(rng, shape, scale, most, pieces=(), kind=jnp.bfloat16):
    loudness = steps_of(rng, shape, pieces, -0.22, 0.18) if pieces else 1.0
    entries = jax.random.normal(rng, shape, jnp.float32) * scale * loudness
    return jnp.minimum(jnp.maximum(entries, -most), most).astype(kind)


def setup_inputs(seed: int = 0, part: int = 0) -> dict:
    keys = jax.random.split(jax.random.key(seed), 10)
    own_keys = jax.random.split(jax.random.fold_in(keys[9], part), 10)
    return {
        "stream": gaussian(own_keys[0], (D, TOKENS), 1.0, 6.0, ((1, 4),)),
        "norm_gain": jnp.clip(1.0 + 0.18 * jax.random.normal(keys[1], (LAYERS, D), jnp.float32), 0.1, 1.9),
        "value_weight": gaussian(keys[2], (LAYERS, C, D), D ** -0.5, 0.09375, ((1, 4),)),
        "gate_weight": gaussian(keys[3], (LAYERS, C, D), D ** -0.5, 0.09375, ((1, 4),)),
        "conv_kernel": draw_conv_kernel(jax.random.fold_in(keys[9], 71), part),
        "conv_bias": gaussian(keys[5], (LAYERS, C), 0.5, 3.0, ((1, 4),), jnp.float32),
        "channel_gain": jnp.clip(1.0 + 0.18 * jax.random.normal(keys[6], (LAYERS, C), jnp.float32), 0.1, 1.9),
        "channel_bias": gaussian(keys[7], (LAYERS, C), 0.5, 3.0, ((1, 4),), jnp.float32),
        "out_weight": gaussian(keys[8], (LAYERS, D, C), (C // 4) ** -0.5, 0.25, ((1, 4),)),
    }


epsilon = 1e-06

def depthwise(signal, kernel):
    length = signal.shape[0]
    padded = jnp.pad(signal, ((K - 1, 0), (0, 0)))
    total = jnp.zeros_like(signal)
    for tap in range(K):
        total = total + padded[tap:tap + length] * kernel[:, tap][None, :]
    return total

def reference(stream, norm_gain, value_weight, gate_weight, conv_kernel, conv_bias, channel_gain, channel_bias, out_weight):
    rows = stream.T
    for layer in range(LAYERS):
        current = rows.astype(jnp.float32)
        scaling = lax.rsqrt(lax.optimization_barrier(jnp.mean(current * current, axis=1, keepdims=True)) + epsilon)
        normed = (current * scaling * norm_gain[layer]).astype(jnp.bfloat16)
        value = jnp.dot(normed, value_weight[layer].T, preferred_element_type=jnp.float32)
        gate_part = jnp.dot(normed, gate_weight[layer].T, preferred_element_type=jnp.float32)
        gated = (value * jax.nn.sigmoid(gate_part)).astype(jnp.bfloat16)
        filtered = depthwise(gated.astype(jnp.float32), conv_kernel[layer]) + conv_bias[layer]
        row_mean = lax.optimization_barrier(jnp.mean(filtered, axis=1, keepdims=True))
        centred = filtered - row_mean
        spread = lax.optimization_barrier(jnp.mean(centred * centred, axis=1, keepdims=True))
        activated = jax.nn.silu(centred * lax.rsqrt(spread + epsilon) * channel_gain[layer] + channel_bias[layer]).astype(jnp.bfloat16)
        branch = jnp.dot(activated, out_weight[layer].T, preferred_element_type=jnp.float32)
        rows = (current + branch).astype(jnp.bfloat16)
    return rows.T
```

```python
import jax
import jax.numpy as jnp
from jax import lax
from jax.sharding import PartitionSpec as P

K = 31
LAYERS = 2
epsilon = 1e-06


def shifted(value, axis, steps):
    count = lax.axis_size(axis)
    initial, last = (max(0, -steps), min(count, count - steps))
    return lax.ppermute(value, axis, [(source, source + steps) for source in range(initial, last)])


def swap(value, bit):
    count = lax.axis_size("tp")
    return lax.ppermute(value, "tp", [(source, source ^ bit) for source in range(count)])


def gather_xor(pieces):
    blocks = {0: list(pieces)}
    bit = lax.axis_size("tp") // 2
    while bit:
        for j in sorted(blocks):
            blocks[j ^ bit] = [swap(piece, bit) for piece in blocks[j]]
        bit //= 2
    return blocks


def depthwise(signal, kernel):
    out = lax.conv_general_dilated(
        signal[None],
        kernel[:, None, :],
        (1,),
        [(0, 0)],
        dimension_numbers=("NCW", "OIW", "NCW"),
        feature_group_count=kernel.shape[0],
        precision=lax.Precision.HIGHEST,
    )
    return out[0]


def dot(a, b):
    return jnp.dot(a, b, preferred_element_type=jnp.float32)


def local(
    stream,
    norm_gain,
    value_weight,
    gate_weight,
    conv_kernel,
    conv_bias,
    channel_gain,
    channel_bias,
    out_weight,
):
    bf16 = jnp.bfloat16
    shard_channels = value_weight.shape[1]
    count = lax.axis_size("tp")
    index = lax.axis_index("tp")
    total_channels = shard_channels * count
    shard_features = out_weight.shape[1]
    features = shard_features * count
    tokens_here = stream.shape[1]

    affine = jnp.concatenate((channel_gain, channel_bias), axis=0)
    affine_blocks = {j: b[0] for j, b in gather_xor([affine]).items()}

    current = lax.dynamic_slice_in_dim(stream, index * shard_features, shard_features, 0)
    current = current.astype(jnp.float32)
    layer_out = None
    for layer in range(LAYERS):
        gain = norm_gain[layer][:, None]
        if layer == 0:
            whole = stream.astype(jnp.float32)
            scaling = lax.rsqrt(jnp.mean(whole * whole, axis=0, keepdims=True) + epsilon)
            normed = (whole * scaling * gain).astype(bf16)
            value = dot(value_weight[layer], normed)
            gate = dot(gate_weight[layer], normed)
        else:
            blocks = gather_xor(layer_out)
            rows = layer_out[0].shape[0]
            square_sum = 0.0
            value = 0.0
            gate = 0.0
            for j in sorted(blocks, key=lambda j: (j & 2, j)):
                for p, piece in enumerate(blocks[j]):
                    start = (index ^ j) * shard_features + p * rows
                    part = piece.astype(jnp.float32)
                    square_sum = square_sum + jnp.sum(part * part, axis=0, keepdims=True)
                    scaled = (part * lax.dynamic_slice_in_dim(gain, start, rows, 0)).astype(bf16)
                    value = value + dot(
                        lax.dynamic_slice_in_dim(value_weight[layer], start, rows, 1), scaled
                    )
                    gate = gate + dot(
                        lax.dynamic_slice_in_dim(gate_weight[layer], start, rows, 1), scaled
                    )
            scaling = lax.rsqrt(square_sum / features + epsilon)
            value = value * scaling
            gate = gate * scaling
        gated = (value * jax.nn.sigmoid(gate)).astype(bf16)
        earlier = shifted(gated[:, tokens_here - (K - 1) :], "sp", 1)
        extended = jnp.concatenate((earlier, gated), axis=1).astype(jnp.float32)
        filtered = depthwise(extended, conv_kernel[layer]) + conv_bias[layer][:, None]
        near_mean = jnp.mean(filtered, axis=0, keepdims=True).astype(bf16)
        offset = (filtered - near_mean.astype(jnp.float32)).astype(bf16)
        blocks = gather_xor([offset, near_mean])
        first_sum = 0.0
        for j, (part, mean) in blocks.items():
            first_sum = first_sum + (
                jnp.sum(part.astype(jnp.float32), axis=0, keepdims=True)
                + mean.astype(jnp.float32) * shard_channels
            )
        row_mean = first_sum / total_channels
        square_sum = 0.0
        for j, (part, mean) in blocks.items():
            centred = part.astype(jnp.float32) + (mean.astype(jnp.float32) - row_mean)
            square_sum = square_sum + jnp.sum(centred * centred, axis=0, keepdims=True)
        scaling = lax.rsqrt(square_sum / total_channels + epsilon)
        branch = 0.0
        for j, (part, mean) in blocks.items():
            centred = part.astype(jnp.float32) + (mean.astype(jnp.float32) - row_mean)
            activated = jax.nn.silu(
                centred * scaling * affine_blocks[j][layer][:, None]
                + affine_blocks[j][LAYERS + layer][:, None]
            ).astype(bf16)
            columns = lax.dynamic_slice_in_dim(
                out_weight[layer], (index ^ j) * shard_channels, shard_channels, 1
            )
            branch = branch + dot(columns, activated)
        result = (current + branch).astype(bf16)
        current = result.astype(jnp.float32)
        half = shard_features // 2
        layer_out = [result[:half], result[half:]]
    return result


def solution(mesh):
    placed = (
        P(None, ("grp", "sp")),
        P(),
        P(None, "tp", None),
        P(None, "tp", None),
        P(None, "tp", None),
        P(None, "tp"),
        P(None, "tp"),
        P(None, "tp"),
        P(None, "tp", None),
    )
    return jax.shard_map(
        local, mesh=mesh, in_specs=placed, out_specs=P("tp", ("grp", "sp")), check_vma=False
    )
```

```python
import jax
import jax.numpy as jnp
from jax import lax
from jax.sharding import PartitionSpec as P

K = 31
LAYERS = 2
epsilon = 1e-06


def shifted(value, axis, steps):
    count = lax.axis_size(axis)
    initial, last = (max(0, -steps), min(count, count - steps))
    return lax.ppermute(value, axis, [(source, source + steps) for source in range(initial, last)])


def swap(value, bit):
    count = lax.axis_size("tp")
    return lax.ppermute(value, "tp", [(source, source ^ bit) for source in range(count)])


def gather_xor(pieces):
    blocks = {0: list(pieces)}
    bit = lax.axis_size("tp") // 2
    while bit:
        for j in sorted(blocks):
            blocks[j ^ bit] = [swap(piece, bit) for piece in blocks[j]]
        bit //= 2
    return blocks


def depthwise(signal, kernel):
    out = lax.conv_general_dilated(
        signal[None],
        kernel[:, None, :],
        (1,),
        [(0, 0)],
        dimension_numbers=("NCW", "OIW", "NCW"),
        feature_group_count=kernel.shape[0],
        precision=lax.Precision.HIGHEST,
    )
    return out[0]


def dot(a, b):
    return jnp.dot(a, b, preferred_element_type=jnp.float32)


def local(
    stream,
    norm_gain,
    value_weight,
    gate_weight,
    conv_kernel,
    conv_bias,
    channel_gain,
    channel_bias,
    out_weight,
):
    bf16 = jnp.bfloat16
    shard_channels = value_weight.shape[1]
    count = lax.axis_size("tp")
    index = lax.axis_index("tp")
    total_channels = shard_channels * count
    shard_features = out_weight.shape[1]
    features = shard_features * count
    tokens_here = stream.shape[1]

    affine = jnp.concatenate((channel_gain, channel_bias), axis=0)
    affine_blocks = {j: b[0] for j, b in gather_xor([affine]).items()}

    def weight_block(weights, layer, start, width):
        block = lax.dynamic_slice(weights, (layer, 0, start), (1, weights.shape[1], width))
        return block[0]

    halo = K - 1
    chunks = 2 if tokens_here % 2 == 0 and tokens_here // 2 >= halo else 1
    span = tokens_here // chunks
    order = list(range(chunks))[::-1]

    current = lax.dynamic_slice_in_dim(stream, index * shard_features, shard_features, 0)
    current = current.astype(jnp.float32)
    current = [current[:, c * span : (c + 1) * span] for c in range(chunks)]
    layer_out = [None] * chunks
    for layer in range(LAYERS):
        gain = norm_gain[layer][:, None]
        gated = [None] * chunks
        if layer == 0:
            whole = stream.astype(jnp.float32)
            scaling = lax.rsqrt(jnp.mean(whole * whole, axis=0, keepdims=True) + epsilon)
            normed = (whole * scaling * gain).astype(bf16)
            value = dot(value_weight[layer], normed)
            gate = dot(gate_weight[layer], normed)
            both = (value * jax.nn.sigmoid(gate)).astype(bf16)
            gated = [both[:, c * span : (c + 1) * span] for c in range(chunks)]
        else:
            arrived = {c: gather_xor([layer_out[c]]) for c in order}
            for c in order:
                square_sum = 0.0
                value = 0.0
                gate = 0.0
                for j in sorted(arrived[c], key=lambda j: (j & 2, j)):
                    start = (index ^ j) * shard_features
                    part = arrived[c][j][0].astype(jnp.float32)
                    square_sum = square_sum + jnp.sum(part * part, axis=0, keepdims=True)
                    part_gain = lax.dynamic_slice_in_dim(gain, start, shard_features, 0)
                    scaled = (part * part_gain).astype(bf16)
                    value = value + dot(
                        weight_block(value_weight, layer, start, shard_features), scaled
                    )
                    gate = gate + dot(
                        weight_block(gate_weight, layer, start, shard_features), scaled
                    )
                scaling = lax.rsqrt(square_sum / features + epsilon)
                gated[c] = (value * scaling * jax.nn.sigmoid(gate * scaling)).astype(bf16)
        before = shifted(gated[-1][:, span - halo :], "sp", 1)
        blocks = [None] * chunks
        for c in order:
            earlier = before if c == 0 else gated[c - 1][:, span - halo :]
            extended = jnp.concatenate((earlier, gated[c]), axis=1).astype(jnp.float32)
            filtered = depthwise(extended, conv_kernel[layer]) + conv_bias[layer][:, None]
            near_mean = jnp.mean(filtered, axis=0, keepdims=True).astype(bf16)
            offset = (filtered - near_mean.astype(jnp.float32)).astype(bf16)
            blocks[c] = gather_xor([offset, near_mean])
        for c in order:
            first_sum = 0.0
            for j, (part, mean) in blocks[c].items():
                first_sum = first_sum + (
                    jnp.sum(part.astype(jnp.float32), axis=0, keepdims=True)
                    + mean.astype(jnp.float32) * shard_channels
                )
            row_mean = first_sum / total_channels
            square_sum = 0.0
            for j, (part, mean) in blocks[c].items():
                centred = part.astype(jnp.float32) + (mean.astype(jnp.float32) - row_mean)
                square_sum = square_sum + jnp.sum(centred * centred, axis=0, keepdims=True)
            scaling = lax.rsqrt(square_sum / total_channels + epsilon)
            branch = 0.0
            for j, (part, mean) in blocks[c].items():
                centred = part.astype(jnp.float32) + (mean.astype(jnp.float32) - row_mean)
                activated = jax.nn.silu(
                    centred * scaling * affine_blocks[j][layer][:, None]
                    + affine_blocks[j][LAYERS + layer][:, None]
                ).astype(bf16)
                columns = weight_block(
                    out_weight, layer, (index ^ j) * shard_channels, shard_channels
                )
                branch = branch + dot(columns, activated)
            layer_out[c] = (current[c] + branch).astype(bf16)
            current[c] = layer_out[c].astype(jnp.float32)
    return jnp.concatenate(layer_out, axis=1)


def solution(mesh):
    placed = (
        P(None, ("grp", "sp")),
        P(),
        P(None, "tp", None),
        P(None, "tp", None),
        P(None, "tp", None),
        P(None, "tp"),
        P(None, "tp"),
        P(None, "tp"),
        P(None, "tp", None),
    )
    return jax.shard_map(
        local, mesh=mesh, in_specs=placed, out_specs=P("tp", ("grp", "sp")), check_vma=False
    )
```

```python
import jax
import jax.numpy as jnp
from jax import lax
from jax.sharding import PartitionSpec as P

K = 31
LAYERS = 2
epsilon = 1e-06


def shifted(value, axis, steps):
    count = lax.axis_size(axis)
    initial, last = (max(0, -steps), min(count, count - steps))
    return lax.ppermute(value, axis, [(source, source + steps) for source in range(initial, last)])


def swap(value, bit):
    count = lax.axis_size("tp")
    return lax.ppermute(value, "tp", [(source, source ^ bit) for source in range(count)])


def gather_xor(pieces):
    blocks = {0: list(pieces)}
    bit = lax.axis_size("tp") // 2
    while bit:
        for j in sorted(blocks):
            blocks[j ^ bit] = [swap(piece, bit) for piece in blocks[j]]
        bit //= 2
    return blocks


def depthwise(signal, kernel):
    out = lax.conv_general_dilated(
        signal[None],
        kernel[:, None, :],
        (1,),
        [(0, 0)],
        dimension_numbers=("NCW", "OIW", "NCW"),
        feature_group_count=kernel.shape[0],
        precision=lax.Precision.HIGHEST,
    )
    return out[0]


def dot(a, b):
    return jnp.dot(a, b, preferred_element_type=jnp.float32)


def local(
    stream,
    norm_gain,
    value_weight,
    gate_weight,
    conv_kernel,
    conv_bias,
    channel_gain,
    channel_bias,
    out_weight,
):
    bf16 = jnp.bfloat16
    shard_channels = value_weight.shape[1]
    count = lax.axis_size("tp")
    index = lax.axis_index("tp")
    total_channels = shard_channels * count
    shard_features = out_weight.shape[1]
    features = shard_features * count
    tokens_here = stream.shape[1]

    affine = jnp.concatenate((channel_gain, channel_bias), axis=0)
    affine_blocks = {j: b[0] for j, b in gather_xor([affine]).items()}

    def weight_block(weights, layer, start, width):
        block = lax.dynamic_slice(weights, (layer, 0, start), (1, weights.shape[1], width))
        return block[0]

    halo = K - 1
    top = count // 2
    chunks = 2 if tokens_here % 2 == 0 and tokens_here // 2 >= halo else 1
    span = tokens_here // chunks
    order = list(range(chunks))[::-1]

    current = lax.dynamic_slice_in_dim(stream, index * shard_features, shard_features, 0)
    current = current.astype(jnp.float32)
    current = [current[:, c * span : (c + 1) * span] for c in range(chunks)]
    layer_out = [None] * chunks
    for layer in range(LAYERS):
        gain = norm_gain[layer][:, None]
        gated = [None] * chunks
        if layer == 0:
            whole = stream.astype(jnp.float32)
            scaling = lax.rsqrt(jnp.mean(whole * whole, axis=0, keepdims=True) + epsilon)
            normed = (whole * scaling * gain).astype(bf16)
            value = dot(value_weight[layer], normed)
            gate = dot(gate_weight[layer], normed)
            both = (value * jax.nn.sigmoid(gate)).astype(bf16)
            gated = [both[:, c * span : (c + 1) * span] for c in range(chunks)]
        else:
            arrived = {c: gather_xor([layer_out[c]]) for c in order}
            for c in order:
                square_sum = 0.0
                value = 0.0
                gate = 0.0
                for j in sorted(arrived[c], key=lambda j: (j & 2, j)):
                    start = (index ^ j) * shard_features
                    part = arrived[c][j][0].astype(jnp.float32)
                    square_sum = square_sum + jnp.sum(part * part, axis=0, keepdims=True)
                    part_gain = lax.dynamic_slice_in_dim(gain, start, shard_features, 0)
                    scaled = (part * part_gain).astype(bf16)
                    value = value + dot(
                        weight_block(value_weight, layer, start, shard_features), scaled
                    )
                    gate = gate + dot(
                        weight_block(gate_weight, layer, start, shard_features), scaled
                    )
                scaling = lax.rsqrt(square_sum / features + epsilon)
                gated[c] = (value * scaling * jax.nn.sigmoid(gate * scaling)).astype(bf16)
        before = shifted(gated[-1][:, span - halo :], "sp", 1)
        blocks = [None] * chunks
        payloads = [None] * chunks
        for c in order:
            earlier = before if c == 0 else gated[c - 1][:, span - halo :]
            extended = jnp.concatenate((earlier, gated[c]), axis=1).astype(jnp.float32)
            filtered = depthwise(extended, conv_kernel[layer]) + conv_bias[layer][:, None]
            near_mean = jnp.mean(filtered, axis=0).astype(bf16)
            offset = (filtered - near_mean.astype(jnp.float32)[None, :]).astype(bf16)
            extra = -(-span // shard_channels)
            tail = jnp.pad(near_mean, (0, extra * shard_channels - span))
            tail = tail.reshape(extra, shard_channels).T
            payloads[c] = jnp.concatenate((offset, tail), axis=1)
            blocks[c] = {0: payloads[c], top: swap(payloads[c], top)} if top else {0: payloads[c]}
        columns = {
            j: weight_block(out_weight, layer, (index ^ j) * shard_channels, shard_channels)
            for j in range(count)
        }
        if layer == 0:
            columns = lax.optimization_barrier(columns)
        done = None
        for c in order:
            if done is not None and top:
                blocks[c][top], done = lax.optimization_barrier((blocks[c][top], done))
                layer_out[order[0]] = done
            bit = top // 2
            while bit:
                for j in sorted(blocks[c]):
                    blocks[c][j ^ bit] = swap(blocks[c][j], bit)
                bit //= 2
            parts = {}
            for j, block in blocks[c].items():
                mean = block[:, span:].T.reshape(-1)[:span].astype(jnp.float32)[None, :]
                parts[j] = (block[:, :span].astype(jnp.float32), mean)
            first_sum = 0.0
            for j, (part, mean) in parts.items():
                first_sum = first_sum + (
                    jnp.sum(part, axis=0, keepdims=True) + mean * shard_channels
                )
            row_mean = first_sum / total_channels
            square_sum = 0.0
            for j, (part, mean) in parts.items():
                centred = part + (mean - row_mean)
                square_sum = square_sum + jnp.sum(centred * centred, axis=0, keepdims=True)
            scaling = lax.rsqrt(square_sum / total_channels + epsilon)
            branch = 0.0
            for j, (part, mean) in parts.items():
                centred = part + (mean - row_mean)
                activated = jax.nn.silu(
                    centred * scaling * affine_blocks[j][layer][:, None]
                    + affine_blocks[j][LAYERS + layer][:, None]
                ).astype(bf16)
                branch = branch + dot(columns[j], activated)
            layer_out[c] = (current[c] + branch).astype(bf16)
            current[c] = layer_out[c].astype(jnp.float32)
            done = layer_out[c]
    return jnp.concatenate(layer_out, axis=1)


def solution(mesh):
    placed = (
        P(None, ("grp", "sp")),
        P(),
        P(None, "tp", None),
        P(None, "tp", None),
        P(None, "tp", None),
        P(None, "tp"),
        P(None, "tp"),
        P(None, "tp"),
        P(None, "tp", None),
    )
    return jax.shard_map(
        local, mesh=mesh, in_specs=placed, out_specs=P("tp", ("grp", "sp")), check_vma=False
    )
```
